256 devices in a mesh: grp: 2 (over y), sp: 16 (over z), tp: 8 (over x, core).
Axes of the slice: x: 4, y: 2, z: 16, core: 2. Of those that a mesh axis runs over, the one named last changes fastest.
The devices are a block of a 4x16x16 slice.
Arguments:
- latents: bfloat16 [8192, 4, 2048], P(('sp', 'tp'), 'grp'), parts along dimension 1, may hold values from -6 to 6
- context: bfloat16 [1024, 4, 2048], P('sp', 'grp'), parts along dimension 1, may hold values from -6 to 6
- condition: float32 [4, 2048], P('grp', 'sp'), parts along dimension 0, may hold values from -6 to 6
- cond_context: float32 [2048], P('sp'), may hold values from -6 to 6
- w_shift: bfloat16 [2048, 2048], P('sp', 'tp'), may hold values from -0.125 to 0.125
- w_scale: bfloat16 [2048, 2048], P('sp', 'tp'), may hold values from -0.125 to 0.125
- w_gate: bfloat16 [2048, 2048], P('sp', 'tp'), may hold values from -0.375 to 0.375
- norm_gain: float32 [2048], replicated, may hold values from 0.1 to 1.9
- w_query: bfloat16 [2048, 1024], P(None, 'tp'), may hold values from -0.375 to 0.375
- w_key: bfloat16 [2048, 512], P(None, 'tp'), may hold values from -0.125 to 0.125
- w_value: bfloat16 [2048, 512], P(None, 'tp'), may hold values from -0.25 to 0.25
- sink_logit: float32 [16], P('tp'), may hold values from 6 to 240
- w_out: bfloat16 [1024, 2048], P('tp'), may hold values from -0.1875 to 0.1875
Outputs:
- refined: bfloat16 [8192, 4, 2048], P(('sp', 'tp'), 'grp'), parts along dimension 1
The draws below stay inside these ranges and needn't reach their ends.
There are 2 independent parts, one for each index of `grp`. The reference program is written for one: setup_inputs(seed, part) draws one part's arguments, and reference() takes and returns one part's arrays. A program takes and returns all parts, laid end to end along the dimension named above; an argument that names none is the same for every part. Nothing has to cross between parts.
All inputs are finite; a program needn't handle non-finite values.
Results may differ from the reference program's by a relative error of at most 0.017.
Values may be sent and summed in bfloat16 or wider, within the bound.
A program may use at most 128 MiB of HBM per device.

```python
import jax
import jax.numpy as jnp
from jax import lax

D = 2048
N_HEADS = 16
N_KV = 8
HEAD_DIM = 64
WINDOW = 128
GRID_W = 64
CTX = 1024
SAMPLES = 2
TOK_DEV = 512
LATENT = 8192
N_TP = 8


def draw_sink_logit(key, part):
    key_base = jax.random.fold_in(key, 11)
    low_sinks = jax.random.uniform(jax.random.fold_in(key_base, 1), (N_HEADS,), jnp.float32, 6.0, 12.0)
    return low_sinks


def shard_levels(stream_key, shape, shards, low, high):
    def one(axis_at, parts):
        steps = jax.random.uniform(jax.random.fold_in(jax.random.fold_in(stream_key, 6), axis_at), (parts,), jnp.float32, low / len(shards), high / len(shards))
        return jnp.repeat(jnp.exp(steps), shape[axis_at] // parts).reshape((-1,) + (1,) * (len(shape) - axis_at - 1))

    factor_of = one(*shards[0])
    for cut in shards[1:]:
        factor_of = factor_of * one(*cut)
    return factor_of


def normal_values(rng, dims, spread, most, split=(), held_as=jnp.bfloat16):
    level = shard_levels(rng, dims, split, -0.22, 0.18) if split else 1.0
    entries = jax.random.normal(rng, dims, jnp.float32) * spread * level
    return jnp.minimum(jnp.maximum(entries, -most), most).astype(held_as)


def setup_inputs(seed: int = 0, part: int = 0) -> dict:
    streams_of = jax.random.split(jax.random.key(seed), 14)
    part_keys = jax.random.split(jax.random.fold_in(streams_of[13], part), 14)
    return {
        "latents": normal_values(part_keys[0], (LATENT, SAMPLES, D), 1.0, 6.0, ((0, 128),)),
        "context": normal_values(part_keys[1], (CTX, SAMPLES, D), 1.0, 6.0, ((0, 16),)),
        "condition": normal_values(part_keys[2], (SAMPLES, D), 1.0, 6.0, ((1, 16),), jnp.float32),
        "cond_context": normal_values(streams_of[3], (D,), 1.0, 6.0, ((0, 16),), jnp.float32),
        "w_shift": normal_values(streams_of[4], (D, D), D ** -0.5, 0.125, ((0, 16), (1, 8))),
        "w_scale": normal_values(streams_of[5], (D, D), D ** -0.5, 0.125, ((0, 16), (1, 8))),
        "w_gate": normal_values(streams_of[6], (D, D), (D // 8) ** -0.5, 0.375, ((0, 16), (1, 8))),
        "norm_gain": jnp.clip(1.0 + 0.18 * jax.random.normal(streams_of[7], (D,), jnp.float32), 0.1, 1.9),
        "w_query": normal_values(streams_of[8], (D, N_HEADS * HEAD_DIM), (D // 8) ** -0.5, 0.375, ((1, 8),)),
        "w_key": normal_values(streams_of[9], (D, N_KV * HEAD_DIM), D ** -0.5, 0.125, ((1, 8),)),
        "w_value": normal_values(streams_of[10], (D, N_KV * HEAD_DIM), (D // 4) ** -0.5, 0.25, ((1, 8),)),
        "sink_logit": draw_sink_logit(jax.random.fold_in(streams_of[13], 71), part),
        "w_out": normal_values(streams_of[12], (N_HEADS * HEAD_DIM, D), (N_HEADS * HEAD_DIM) ** -0.5, 0.1875, ((0, 8),)),
    }


EPS = 1e-06
THETA = 10000.0
BIG_NEG = -1e+30

def rotate_pairs(vectors, grid_row, grid_col, head_dim):
    quarter = head_dim // 4
    inverse = THETA ** (-jnp.arange(quarter, dtype=jnp.float32) / quarter)
    angles = jnp.concatenate([grid_row[:, None] * inverse, grid_col[:, None] * inverse], axis=-1)
    shape = (angles.shape[0],) + (1,) * (vectors.ndim - 2) + (head_dim // 2,)
    cosine = jnp.cos(angles).reshape(shape)
    sine = jnp.sin(angles).reshape(shape)
    first_half = vectors[..., :head_dim // 2]
    second_half = vectors[..., head_dim // 2:]
    return jnp.concatenate([first_half * cosine - second_half * sine, first_half * sine + second_half * cosine], axis=-1)

def modulate(tokens_in, gain, shift_rows, scale_rows):
    upcast = tokens_in.astype(jnp.float32)
    normed = upcast * lax.rsqrt(lax.optimization_barrier(jnp.mean(upcast * upcast, axis=-1, keepdims=True)) + EPS)
    return (normed * gain * (1.0 + scale_rows) + shift_rows).astype(jnp.bfloat16)

def reference(latents, context, condition, cond_context, w_shift, w_scale, w_gate, norm_gain, w_query, w_key, w_value, sink_logit, w_out):
    lifted = jax.nn.silu(jnp.concatenate([condition, cond_context[None, :]], axis=0)).astype(jnp.bfloat16)
    shift_all = jnp.dot(lifted, w_shift, preferred_element_type=jnp.float32)
    scale_all = jnp.dot(lifted, w_scale, preferred_element_type=jnp.float32)
    gate_all = jnp.dot(lifted, w_gate, preferred_element_type=jnp.float32)
    normed = modulate(latents, norm_gain, shift_all[:SAMPLES][None], scale_all[:SAMPLES][None])
    ctx_normed = modulate(context, norm_gain, shift_all[SAMPLES][None, None], scale_all[SAMPLES][None, None])
    flat_rows = normed.reshape(LATENT * SAMPLES, D)
    positions = jnp.arange(LATENT, dtype=jnp.int32)
    grid_row = (positions // GRID_W).astype(jnp.float32)
    grid_col = (positions % GRID_W).astype(jnp.float32)
    q_full = jnp.dot(flat_rows, w_query, preferred_element_type=jnp.float32).reshape(LATENT, SAMPLES, N_HEADS, HEAD_DIM)
    k_full = jnp.dot(flat_rows, w_key, preferred_element_type=jnp.float32).reshape(LATENT, SAMPLES, N_KV, HEAD_DIM)
    queries = rotate_pairs(q_full, grid_row, grid_col, HEAD_DIM).astype(jnp.bfloat16)
    lat_keys = rotate_pairs(k_full, grid_row, grid_col, HEAD_DIM).astype(jnp.bfloat16)
    lat_values = jnp.dot(flat_rows, w_value, preferred_element_type=jnp.float32).astype(jnp.bfloat16).reshape(LATENT, SAMPLES, N_KV, HEAD_DIM)
    ctx_flat = ctx_normed.reshape(CTX * SAMPLES, D)
    ctx_keys = jnp.dot(ctx_flat, w_key, preferred_element_type=jnp.float32).astype(jnp.bfloat16).reshape(CTX, SAMPLES, N_KV, HEAD_DIM)
    ctx_values = jnp.dot(ctx_flat, w_value, preferred_element_type=jnp.float32).astype(jnp.bfloat16).reshape(CTX, SAMPLES, N_KV, HEAD_DIM)
    per_group = N_HEADS // N_KV
    block_rows = min(TOK_DEV, 256)
    n_blocks = LATENT // block_rows
    padding = ((WINDOW, WINDOW), (0, 0), (0, 0), (0, 0))
    keys_padded = jnp.pad(lat_keys, padding)
    values_padded = jnp.pad(lat_values, padding)
    head_sinks = sink_logit.astype(jnp.float32).reshape(N_KV, per_group)
    score_scale = HEAD_DIM ** (-0.5)
    ctx_k32 = ctx_keys.astype(jnp.float32)
    ctx_v32 = ctx_values.astype(jnp.float32)

    def attend_block(block_index):
        first_row = block_index * block_rows
        q_blk = lax.dynamic_slice_in_dim(queries, first_row, block_rows, 0).reshape(block_rows, SAMPLES, N_KV, per_group, HEAD_DIM).astype(jnp.float32)
        k_blk = lax.dynamic_slice_in_dim(keys_padded, first_row, block_rows + 2 * WINDOW, 0).astype(jnp.float32)
        v_blk = lax.dynamic_slice_in_dim(values_padded, first_row, block_rows + 2 * WINDOW, 0).astype(jnp.float32)
        lat_scores = jnp.einsum('qsngd,ksnd->sngqk', q_blk, k_blk) * score_scale
        q_pos = first_row + jnp.arange(block_rows, dtype=jnp.int32)
        k_pos = first_row - WINDOW + jnp.arange(block_rows + 2 * WINDOW, dtype=jnp.int32)
        in_window = (jnp.abs(q_pos[:, None] - k_pos[None, :]) <= WINDOW) & (k_pos >= 0)[None, :] & (k_pos < LATENT)[None, :]
        lat_scores = jnp.where(in_window, lat_scores, BIG_NEG)
        ctx_scores = jnp.einsum('qsngd,ksnd->sngqk', q_blk, ctx_k32) * score_scale
        sink_col = jnp.broadcast_to(head_sinks[None, :, :, None, None], lat_scores.shape[:-1] + (1,))
        joined = jax.nn.softmax(jnp.concatenate([lat_scores, ctx_scores, sink_col], axis=-1), axis=-1)
        weights_low = joined.astype(jnp.bfloat16).astype(jnp.float32)
        lat_part = weights_low[..., :block_rows + 2 * WINDOW]
        ctx_part = weights_low[..., block_rows + 2 * WINDOW:block_rows + 2 * WINDOW + CTX]
        summed = jnp.einsum('sngqk,ksnd->qsngd', lat_part, v_blk) + jnp.einsum('sngqk,ksnd->qsngd', ctx_part, ctx_v32)
        return summed.astype(jnp.bfloat16).reshape(block_rows, SAMPLES, N_HEADS * HEAD_DIM)
    attended = lax.map(attend_block, jnp.arange(n_blocks)).reshape(LATENT * SAMPLES, N_HEADS * HEAD_DIM)
    group_cols = N_HEADS * HEAD_DIM // N_TP
    mixed = jnp.zeros((LATENT * SAMPLES, D), jnp.float32)
    for group_index in range(N_TP):
        lo_col = group_index * group_cols
        partial_term = jnp.dot(attended[:, lo_col:lo_col + group_cols], w_out[lo_col:lo_col + group_cols], preferred_element_type=jnp.float32)
        rounded = lax.optimization_barrier(partial_term.astype(jnp.bfloat16))
        mixed = mixed + rounded.astype(jnp.float32)
    mixed = mixed.reshape(LATENT, SAMPLES, D)
    refined = latents.astype(jnp.float32) + gate_all[:SAMPLES][None] * mixed
    return refined.astype(jnp.bfloat16)
```

```python
import functools
import math

import jax
import jax.numpy as jnp
import numpy as np
from jax import lax
from jax.experimental import pallas as pl
from jax.experimental.pallas import tpu as pltpu
from jax.sharding import PartitionSpec as P

HEAD_DIM = 64
WINDOW = 128
GRID_W = 64
EPS = 1e-06
THETA = 10000.0
BIG_NEG = -1e30
LOG2E = math.log2(math.e)
MESH = pl.DeviceIdType.MESH
F32 = jnp.float32
BF16 = jnp.bfloat16
LAT_SPLIT = 96


def rope_tables(n_rows):
    quarter = HEAD_DIM // 4
    inverse = (THETA ** (-np.arange(quarter, dtype=np.float32) / np.float32(quarter))).astype(np.float32)
    lane = np.arange(128)
    freq = inverse[lane % quarter]
    by_row = (lane % (HEAD_DIM // 2)) < quarter
    sign = np.where(lane % HEAD_DIM < HEAD_DIM // 2, -1.0, 1.0)

    def tables(positions, mine):
        angle = (positions.astype(np.float32)[:, None] * freq[None, :]).astype(np.float64)
        cosine = np.where(mine[None, :], np.cos(angle), 0.0)
        sine = np.where(mine[None, :], np.sin(angle) * sign[None, :], 0.0)
        return cosine, sine

    def four(positions, mine, ones):
        cosine, sine = tables(positions, mine)
        scale = HEAD_DIM ** (-0.5) * LOG2E
        key = (lane < HEAD_DIM)[None, :]
        return np.stack(
            [cosine * scale, sine * scale, np.where(key, cosine, ones), np.where(key, sine, 0.0)]
        ).astype(np.float32)

    cols = np.repeat(np.arange(GRID_W), 2)
    return four(cols, ~by_row, 1.0), four(np.arange(n_rows), by_row, 0.0)


def remote(src, dst, send_sem, recv_sem, device):
    return pltpu.make_async_remote_copy(
        src_ref=src,
        dst_ref=dst,
        send_sem=send_sem,
        recv_sem=recv_sem,
        device_id=device,
        device_id_type=MESH,
    )


class TwoHopGather:
    def __init__(self, n, me, slot, send_sems, recv_sems):
        self.n, self.me, self.slot = n, me, slot
        self.send_sems, self.recv_sems = send_sems, recv_sems
        self.reach = {1: n // 2, -1: n - 1 - n // 2}
        self.sent, self.pending = [], {}
        for way in (1, -1):
            for e in range(1, self.reach[way] + 1):
                self.pending[(way, e)] = True

    def at(self, way, e):
        return e - 1 if way == 1 else self.reach[1] + e - 1

    def send(self, way, d, e):
        owner = lax.rem(self.me - way * d + self.n, self.n)
        target = lax.rem(self.me + way * (e - d) + self.n, self.n)
        k = self.at(way, e)
        copy = remote(
            self.slot(owner), self.slot(owner), self.send_sems.at[k], self.recv_sems.at[k], {"sp": target}
        )
        copy.start()
        self.sent.append(copy)

    def pass_on(self, d):
        for way in (1, -1):
            if d >= self.reach[way]:
                continue
            if d > 0:
                self.wait(way, d)
            for e in (d + 1, d + 2):
                if e <= self.reach[way]:
                    self.send(way, d, e)

    def wait(self, way, e):
        owner = lax.rem(self.me - way * e + self.n, self.n)
        k = self.at(way, e)
        remote(
            self.slot(owner), self.slot(owner), self.send_sems.at[k], self.recv_sems.at[k], {"sp": self.me}
        ).wait_recv()
        del self.pending[(way, e)]

    def finish(self):
        for way, e in list(self.pending):
            self.wait(way, e)

    def drain(self):
        for copy in self.sent:
            copy.wait_send()


class RingOfChips:
    def __init__(self, buf, me, n, send_sems, recv_sems, pieces):
        self.buf, self.n = buf, n
        self.send_sems, self.recv_sems = send_sems, recv_sems
        self.pieces = pieces
        self.x, self.c = me // 2, lax.rem(me, 2)
        self.chips = n // 2
        self.me = me
        self.partner = me + 1 - 2 * self.c
        self.left_x = lax.rem(self.x + self.chips - 1, self.chips)
        self.right_x = lax.rem(self.x + 1, self.chips)
        self.far_x = lax.rem(self.x + 2, self.chips)
        self.sent = []
        self.base = {}
        k = 0
        for name in ("left", "right"):
            self.base[name] = k
            k += len(pieces)
        for name in ("far", "own2", "left2", "right2", "far2"):
            self.base[name] = k
            k += 1

    @staticmethod
    def count(pieces):
        return 2 * len(pieces) + 5

    def piece(self, owner, p):
        lo, size = self.pieces[p]
        return self.buf.at[owner, pl.ds(lo, size), :]

    def go(self, ref, k, target):
        copy = remote(ref, ref, self.send_sems.at[k], self.recv_sems.at[k], {"tp": target})
        copy.start()
        self.sent.append(copy)

    def land(self, ref, k):
        remote(ref, ref, self.send_sems.at[k], self.recv_sems.at[k], {"tp": self.partner}).wait_recv()

    def send_own(self, p):
        ref = self.piece(self.me, p)
        self.go(ref, self.base["left"] + p, self.right_x * 2 + self.c)
        self.go(ref, self.base["right"] + p, self.left_x * 2 + self.c)

    def share_own(self):
        self.go(self.buf.at[self.me], self.base["own2"], self.partner)

    def pass_near(self):
        left, right = self.left_x * 2 + self.c, self.right_x * 2 + self.c
        for p in range(len(self.pieces)):
            self.land(self.piece(left, p), self.base["left"] + p)
            self.land(self.piece(right, p), self.base["right"] + p)
        from_x = lax.rem(self.x + self.chips - 1 + 2 * self.c, self.chips)
        to_x = lax.rem(self.x + self.chips + 1 - 2 * self.c, self.chips)
        self.go(self.buf.at[from_x * 2 + self.c], self.base["far"], to_x * 2 + self.c)
        self.go(self.buf.at[left], self.base["left2"], self.partner)
        self.go(self.buf.at[right], self.base["right2"], self.partner)

    def pass_far(self):
        far = self.far_x * 2 + self.c
        self.land(self.buf.at[far], self.base["far"])
        self.go(self.buf.at[far], self.base["far2"], self.partner)

    def land_shared(self, name):
        x = {"own2": self.x, "left2": self.left_x, "right2": self.right_x, "far2": self.far_x}[name]
        self.land(self.buf.at[x * 2 + 1 - self.c], self.base[name])

    def drain(self):
        for copy in self.sent:
            copy.wait_send()


def kernel(
    n_sp, n_tp, seq_length,
    lat_hbm, ctx_hbm, cond_hbm, cc_hbm, wsh_hbm, wsc_hbm, wga_hbm, gain_hbm, wq_hbm, wkt_hbm, wvt_hbm, sink_ref,
    wo_hbm, col_hbm, row_hbm,
    out_ref,
    lat_all, wo_all, ctx_v, cond_v, cc_v, wmod_v, gain_v, w_all, wkvt_v, col_v, row_v,
    pm, ms, a16, b16, g16, ac16, bc16, ssq, rsb, rsc, xn, tmp,
    q_s, kv_s, vv_s, ck, cv, o_s, m_s, tmp2, asend, att_all,
    loc, zsend, zrecv, lsend, lrecv, wsend, wrecv, msend, mrecv, hsend, hrecv, asem, arecv,
):
    sp = lax.axis_index("sp")
    tp = lax.axis_index("tp")
    rows = lat_all.shape[1]
    local_tok = rows // 2
    tokens = local_tok * n_tp
    width = lat_all.shape[2]
    mod_cols = pm.shape[2]
    ctx_tok = ctx_v.shape[0] // 2

    lat_x = RingOfChips(lat_all, tp, n_tp, lsend, lrecv, ((0, LAT_SPLIT), (LAT_SPLIT, rows - LAT_SPLIT)))
    wo_x = RingOfChips(wo_all, tp, n_tp, wsend, wrecv, ((0, rows),))
    mods = TwoHopGather(n_sp, sp, lambda o: pm.at[o], zsend.at[0], zrecv.at[0])
    ctxs = TwoHopGather(
        n_sp, sp, lambda o: ck.at[:, pl.ds(pl.multiple_of(o * ctx_tok, ctx_tok), ctx_tok), :], zsend.at[1], zrecv.at[1]
    )

    barrier = pltpu.get_barrier_semaphore()
    near = [d for d in (1, 2, n_sp - 1, n_sp - 2)]
    for d in near:
        pl.semaphore_signal(barrier, inc=1, device_id={"sp": lax.rem(sp + d, n_sp)}, device_id_type=MESH)
    for k in range(1, n_tp):
        pl.semaphore_signal(barrier, inc=1, device_id={"tp": lax.rem(tp + k, n_tp)}, device_id_type=MESH)

    loads = [
        pltpu.make_async_copy(cond_hbm, cond_v, loc.at[0]),
        pltpu.make_async_copy(cc_hbm, cc_v, loc.at[1]),
        pltpu.make_async_copy(wsh_hbm, wmod_v.at[0], loc.at[2]),
        pltpu.make_async_copy(wsc_hbm, wmod_v.at[1], loc.at[3]),
        pltpu.make_async_copy(wga_hbm, wmod_v.at[2], loc.at[4]),
        pltpu.make_async_copy(lat_hbm, lat_all.at[tp], loc.at[5]),
        pltpu.make_async_copy(wkt_hbm, wkvt_v.at[pl.ds(0, HEAD_DIM)], loc.at[6]),
        pltpu.make_async_copy(wvt_hbm, wkvt_v.at[pl.ds(HEAD_DIM, HEAD_DIM)], loc.at[7]),
        pltpu.make_async_copy(wq_hbm, w_all.at[:, pl.ds(0, 128)], loc.at[8]),
        pltpu.make_async_copy(ctx_hbm, ctx_v, loc.at[9]),
        pltpu.make_async_copy(gain_hbm, gain_v, loc.at[10]),
        pltpu.make_async_copy(col_hbm, col_v, loc.at[11]),
        pltpu.make_async_copy(row_hbm.at[:, pl.ds(pl.multiple_of(sp * n_tp, n_tp), n_tp), :], row_v, loc.at[12]),
        pltpu.make_async_copy(wo_hbm, wo_all.at[tp], loc.at[13]),
    ]
    for load in loads:
        load.start()

    for load in loads[:5]:
        load.wait()
    sub = lax.broadcasted_iota(jnp.int32, (8, cond_v.shape[1]), 0)
    kind = lax.rem(sub, 3)
    raw = jnp.where(kind == 0, cond_v[0:1, :], jnp.where(kind == 1, cond_v[1:2, :], cc_v[0:1, :]))
    lifted = raw / (1.0 + jnp.exp(-raw))
    part = jnp.zeros((8, mod_cols), F32)
    for k in range(3):
        mine = (sub >= 3 * k) & (sub < 3 * k + 3)
        part = part + jnp.dot(
            jnp.where(mine, lifted, 0.0).astype(BF16), wmod_v[k], preferred_element_type=F32
        )
    pm[sp] = part

    pl.semaphore_wait(barrier, len(near) + n_tp - 1)
    mods.pass_on(0)
    loads[5].wait()
    lat_x.send_own(0)
    lat_x.share_own()
    for load in loads[6:]:
        load.wait()
    wo_x.share_own()

    w_all[:, 128:256] = wkvt_v[...].T
    mods.pass_on(2)

    def row_scale(load_rows, n_rows, rs_ref):
        def body(i, _):
            at = pl.ds(pl.multiple_of(i * 16, 16), 16)
            x = load_rows(at).astype(F32)
            sq = x * x
            acc = sq[:, 0:128]
            for k in range(1, width // 128):
                acc = acc + sq[:, 128 * k : 128 * k + 128]
            ssq[at, :] = acc
            return 0

        lax.fori_loop(0, n_rows // 16, body, 0)
        total = jnp.sum(ssq[0:n_rows, :], axis=-1, keepdims=True)
        rs_ref[0:n_rows, :] = jnp.broadcast_to(lax.rsqrt(total * (1.0 / width) + EPS), (n_rows, 128))

    def normalise(load_rows, n_rows, rs_ref, a_ref, b_ref):
        def body(i, _):
            at = pl.ds(pl.multiple_of(i * 16, 16), 16)
            x = load_rows(at).astype(F32)
            r = rs_ref[at, :]
            for k in range(width // 128):
                c = slice(128 * k, 128 * k + 128)
                xn[at, c] = (x[:, c] * r * a_ref[:, c] + b_ref[:, c]).astype(BF16)
            return 0

        lax.fori_loop(0, n_rows // 16, body, 0)

    row_scale(lambda at: ctx_v[at, :], 2 * ctx_tok, rsc)
    mods.pass_on(4)
    mods.pass_on(6)
    mods.finish()

    total = pm[0]
    for k in range(1, n_sp):
        total = total + pm[k]
    ms[tp] = total
    m_copies = []
    for k in range(1, n_tp):
        to = lax.rem(tp + k, n_tp)
        copy = remote(ms.at[tp], ms.at[tp], msend.at[k], mrecv.at[k], {"tp": to})
        copy.start()
        m_copies.append(copy)
    lat_x.send_own(1)
    for k in range(1, n_tp):
        source = lax.rem(tp + n_tp - k, n_tp)
        remote(ms.at[source], ms.at[source], msend.at[k], mrecv.at[k], {"tp": tp}).wait_recv()
    par = lax.rem(lax.broadcasted_iota(jnp.int32, (16, mod_cols), 0), 2) == 0
    for t in range(n_tp):
        c = slice(t * mod_cols, (t + 1) * mod_cols)
        m = ms[t]
        gain = gain_v[:, c]
        ac16[:, c] = jnp.broadcast_to(gain * (1.0 + m[5:6]), (16, mod_cols))
        bc16[:, c] = jnp.broadcast_to(m[2:3], (16, mod_cols))
        a16[:, c] = jnp.where(par, gain * (1.0 + m[3:4]), gain * (1.0 + m[4:5]))
        b16[:, c] = jnp.where(par, m[0:1], m[1:2])
        g16[:, c] = jnp.where(par, m[6:7], m[7:8])

    lane_lo = lax.broadcasted_iota(jnp.int32, (64, 128), 1) < HEAD_DIM
    normalise(lambda at: ctx_v[at, :], 2 * ctx_tok, rsc, ac16, bc16)
    tmp[...] = jnp.dot(xn[...], w_all[:, 128:256], preferred_element_type=F32)
    for s in range(2):
        ck[s, pl.ds(pl.multiple_of(sp * ctx_tok, ctx_tok), ctx_tok), :] = tmp[
            pl.ds(s, ctx_tok, stride=2), :
        ].astype(BF16)
    ctxs.pass_on(0)

    lane = lax.broadcasted_iota(jnp.int32, (rows, 128), 1)
    first_half = lax.rem(lane, HEAD_DIM) < HEAD_DIM // 2

    def rotate(v, cos, sin):
        swapped = jnp.where(first_half, pltpu.roll(v, 128 - HEAD_DIM // 2, 1), pltpu.roll(v, HEAD_DIM // 2, 1))
        return v * cos + swapped * sin

    def one_block(b):
        row_scale(lambda at: lat_all[b, at, :], rows, rsb)
        normalise(lambda at: lat_all[b, at, :], rows, rsb, a16, b16)
        proj = jnp.dot(xn[...], w_all[...], preferred_element_type=F32)
        at_q = pl.ds(pl.multiple_of(b * local_tok, local_tok), local_tok)
        at_k = pl.ds(pl.multiple_of(b * local_tok + WINDOW, local_tok), local_tok)
        r = [row_v[k, pl.ds(b, 1), :] for k in range(4)]
        tmp[...] = rotate(proj[:, 0:128], col_v[0] + r[0], col_v[1] + r[1])
        for s in range(2):
            v = tmp[pl.ds(s, local_tok, stride=2), :]
            q_s[s, 0, at_q, :] = jnp.where(lane_lo, v, 0.0).astype(BF16)
            q_s[s, 1, at_q, :] = jnp.where(lane_lo, pltpu.roll(v, 64, 1), 0.0).astype(BF16)
        tmp[...] = rotate(proj[:, 128:256], col_v[2] + r[2], col_v[3] + r[3])
        for s in range(2):
            v = tmp[pl.ds(s, local_tok, stride=2), :]
            kv_s[s, at_k, :] = v.astype(BF16)
            vv_s[s, at_k, :] = jnp.where(lane_lo, 1.0, v).astype(BF16)

    def chip_blocks(x):
        def body(j, _):
            one_block(x * 2 + j)
            return 0

        lax.fori_loop(0, 2, body, 0)

    lat_x.pass_near()
    wo_x.send_own(0)
    lat_x.land_shared("own2")
    chip_blocks(lat_x.x)
    ctxs.pass_on(2)
    lat_x.land_shared("left2")
    chip_blocks(lat_x.left_x)
    ctxs.pass_on(4)
    lat_x.land_shared("right2")
    chip_blocks(lat_x.right_x)
    lat_x.pass_far()
    ctxs.pass_on(6)
    lat_x.land_shared("far2")
    chip_blocks(lat_x.far_x)

    up, down = lax.rem(sp + 1, n_sp), lax.rem(sp + n_sp - 1, n_sp)
    to_down = remote(
        kv_s.at[:, pl.ds(WINDOW, WINDOW), :], kv_s.at[:, pl.ds(tokens + WINDOW, WINDOW), :],
        hsend.at[0], hrecv.at[0], {"sp": down},
    )
    to_up = remote(
        kv_s.at[:, pl.ds(tokens, WINDOW), :], kv_s.at[:, pl.ds(0, WINDOW), :], hsend.at[1], hrecv.at[1], {"sp": up}
    )
    to_down.start()
    to_up.start()
    wo_x.pass_near()
    to_down.wait_recv()
    to_up.wait_recv()
    edge_lo = lax.broadcasted_iota(jnp.int32, (WINDOW, 128), 1) < HEAD_DIM
    one = jnp.ones((WINDOW, 128), BF16)
    for s in range(2):
        for at in (0, tokens + WINDOW):
            vv_s[s, at : at + WINDOW, :] = jnp.where(edge_lo, one, kv_s[s, at : at + WINDOW, :])

    q_rows = WINDOW
    n_q = tokens // q_rows
    heads = q_s.shape[1]
    stack = heads * q_rows
    span = q_rows + 2 * WINDOW
    row_i = lax.broadcasted_iota(jnp.int32, (stack, span), 0)
    i_q = lax.rem(row_i, q_rows)
    j_k = lax.broadcasted_iota(jnp.int32, (stack, span), 1)
    first_head = lax.broadcasted_iota(jnp.int32, (stack, 128), 0) < q_rows
    sink = jnp.where(first_head, sink_ref[0] * LOG2E, sink_ref[1] * LOG2E)
    sum_lane = lax.broadcasted_iota(jnp.int32, (stack, 128), 1) < HEAD_DIM

    def scores(q, k):
        return lax.dot_general(q, k, (((1,), (1,)), ((), ())), preferred_element_type=F32)

    def window_block(it, _):
        s = it // n_q
        qb = lax.rem(it, n_q)
        at_q = pl.ds(pl.multiple_of(qb * q_rows, q_rows), q_rows)
        at_k = pl.ds(pl.multiple_of(qb * q_rows, q_rows), span)
        q = q_s[s, :, at_q, :].reshape(stack, 128)
        first_key = sp * tokens + qb * q_rows - WINDOW
        lo = jnp.maximum(i_q, -first_key)
        hi = jnp.minimum(i_q + 2 * WINDOW, seq_length - 1 - first_key)
        sc = jnp.where((j_k >= lo) & (j_k <= hi), scores(q, kv_s[s, at_k, :]), BIG_NEG)
        top = jnp.maximum(jnp.max(sc, axis=-1, keepdims=True), sink)
        p = jnp.exp2(sc - top[:, 0:1]).astype(BF16)
        o = jnp.dot(p, vv_s[s, at_k, :], preferred_element_type=F32)
        o_s[it] = o + jnp.where(sum_lane, jnp.exp2(sink - top), 0.0)
        m_s[it] = top
        return 0

    lax.fori_loop(0, 2 * n_q, window_block, 0)

    ctxs.finish()
    n_ctx = ck.shape[1]
    ctx_lo = lax.broadcasted_iota(jnp.int32, (n_ctx, 128), 1) < HEAD_DIM
    for s in range(2):
        cv[s] = jnp.where(ctx_lo, jnp.ones((n_ctx, 128), BF16), ck[s])
    out_lo = lax.broadcasted_iota(jnp.int32, (q_rows, 128), 1) < HEAD_DIM

    def a_copy(b):
        return remote(
            asend.at[b], att_all.at[tp], asem.at[b], arecv.at[tp], {"tp": b}
        )

    per_q = q_rows // local_tok

    def ctx_block(qb, _):
        for s in range(2):
            it = s * n_q + qb
            at_q = pl.ds(pl.multiple_of(qb * q_rows, q_rows), q_rows)
            q = q_s[s, :, at_q, :].reshape(stack, 128)
            sc = scores(q, ck[s])
            old = m_s[it]
            top = jnp.maximum(jnp.max(sc, axis=-1, keepdims=True), old)
            p = jnp.exp2(sc - top[:, 0:1]).astype(BF16)
            o = jnp.dot(p, cv[s], preferred_element_type=F32) + o_s[it] * jnp.exp2(old - top)
            r = o / pltpu.roll(o, 64, 1)
            tmp2[pl.ds(s, q_rows, stride=2), :] = jnp.where(
                out_lo, pltpu.roll(r[0:q_rows], 64, 1), r[q_rows:stack]
            )
        for k in range(per_q):
            asend[qb * per_q + k] = tmp2[k * rows : (k + 1) * rows, :].astype(BF16)
        for k in range(per_q):
            b = qb * per_q + k

            @pl.when(b != tp)
            def _():
                a_copy(b).start()

        return 0

    lax.fori_loop(0, n_q, ctx_block, 0)

    wo_x.pass_far()
    att_all[tp] = asend[tp]
    for k in range(1, n_tp):
        source = lax.rem(tp + k, n_tp)
        remote(
            asend.at[0], att_all.at[source], asem.at[0], arecv.at[source], {"tp": tp}
        ).wait_recv()
    for name in ("own2", "left2", "right2", "far2"):
        wo_x.land_shared(name)

    att = jnp.concatenate([att_all[t] for t in range(n_tp)], axis=1)
    tile = 256

    def out_block(n, _):
        c = pl.ds(pl.multiple_of(n * tile, tile), tile)
        w = wo_all[:, :, c].reshape(n_tp * rows, tile)
        mixed = jnp.dot(att, w, preferred_element_type=F32)
        gated = (mixed.reshape(rows // 16, 16, tile) * g16[:, c][None]).reshape(rows, tile)
        out_ref[:, c] = (lat_all[tp, :, c].astype(F32) + gated).astype(BF16)
        return 0

    lax.fori_loop(0, width // tile, out_block, 0)

    mods.drain()
    ctxs.drain()
    lat_x.drain()
    wo_x.drain()
    for copy in m_copies:
        copy.wait_send()
    to_down.wait_send()
    to_up.wait_send()
    for b in range(n_tp):

        @pl.when(b != tp)
        def _():
            a_copy(b).wait_send()


def on_device(n_sp, n_tp, latents, context, condition, cond_context, w_shift, w_scale, w_gate, norm_gain, w_query,
              w_key, w_value, sink_logit, w_out):
    local_tok, samples, width = latents.shape
    ctx_tok = context.shape[0]
    rows, ctx_rows = local_tok * samples, ctx_tok * samples
    tokens = local_tok * n_tp
    n_ctx = ctx_tok * n_sp
    mod_cols = w_shift.shape[1]
    heads = w_query.shape[1] // HEAD_DIM
    assert samples == 2 and local_tok == GRID_W and heads == 2 and w_key.shape[1] == HEAD_DIM
    assert w_out.shape[0] == rows == ctx_rows == 128
    col_tab, row_tab = rope_tables(tokens * n_sp // GRID_W)
    n_blocks = tokens // WINDOW
    any_spec = pl.BlockSpec(memory_space=pl.ANY)
    n_l = RingOfChips.count((0, 0))
    n_w = RingOfChips.count((0,))
    dma = pltpu.SemaphoreType.DMA
    scratch = [
        pltpu.VMEM((n_tp, rows, width), BF16),
        pltpu.VMEM((n_tp, rows, width), BF16),
        pltpu.VMEM((ctx_rows, width), BF16),
        pltpu.VMEM(condition.shape, F32),
        pltpu.VMEM((1, cond_context.shape[0]), F32),
        pltpu.VMEM((3, *w_shift.shape), BF16),
        pltpu.VMEM((1, width), F32),
        pltpu.VMEM((width, 256), BF16),
        pltpu.VMEM((128, width), BF16),
        pltpu.VMEM((4, rows, 128), F32),
        pltpu.VMEM((4, n_tp, 128), F32),
        pltpu.VMEM((n_sp, 8, mod_cols), F32),
        pltpu.VMEM((n_tp, 8, mod_cols), F32),
        *[pltpu.VMEM((16, width), F32) for _ in range(5)],
        *[pltpu.VMEM((rows, 128), F32) for _ in range(3)],
        pltpu.VMEM((rows, width), BF16),
        pltpu.VMEM((rows, 128), F32),
        pltpu.VMEM((2, heads, tokens, 128), BF16),
        pltpu.VMEM((2, tokens + 2 * WINDOW, 128), BF16),
        pltpu.VMEM((2, tokens + 2 * WINDOW, 128), BF16),
        pltpu.VMEM((2, n_ctx, 128), BF16),
        pltpu.VMEM((2, n_ctx, 128), BF16),
        pltpu.VMEM((2 * n_blocks, heads * WINDOW, 128), F32),
        pltpu.VMEM((2 * n_blocks, heads * WINDOW, 128), F32),
        pltpu.VMEM((2 * WINDOW, 128), F32),
        pltpu.VMEM((n_tp, rows, 128), BF16),
        pltpu.VMEM((n_tp, rows, 128), BF16),
        dma((14,)),
        dma((2, n_sp)), dma((2, n_sp)),
        dma((n_l,)), dma((n_l,)),
        dma((n_w,)), dma((n_w,)),
        dma((n_tp,)), dma((n_tp,)),
        dma((2,)), dma((2,)),
        dma((n_tp,)), dma((n_tp,)),
    ]
    out = pl.pallas_call(
        functools.partial(kernel, n_sp, n_tp, tokens * n_sp),
        out_shape=jax.ShapeDtypeStruct((rows, width), BF16),
        in_specs=[any_spec] * 11 + [pl.BlockSpec(memory_space=pltpu.SMEM)] + [any_spec] * 3,
        out_specs=pl.BlockSpec(memory_space=pltpu.VMEM),
        scratch_shapes=scratch,
        compiler_params=pltpu.CompilerParams(
            collective_id=0, has_side_effects=True, vmem_limit_bytes=60 * 1024 * 1024
        ),
    )(
        latents.reshape(rows, width),
        context.reshape(ctx_rows, width),
        condition,
        cond_context[None, :],
        w_shift,
        w_scale,
        w_gate,
        norm_gain[None, :],
        w_query,
        w_key.T,
        w_value.T,
        sink_logit,
        w_out,
        jnp.asarray(col_tab),
        jnp.asarray(row_tab),
    )
    return out.reshape(local_tok, samples, width)


def solution(mesh):
    n_sp, n_tp = mesh.shape["sp"], mesh.shape["tp"]
    sp_tp = ("sp", "tp")
    return jax.shard_map(
        functools.partial(on_device, n_sp, n_tp),
        mesh=mesh,
        in_specs=(
            P(sp_tp, "grp", None),
            P("sp", "grp", None),
            P("grp", "sp"),
            P("sp"),
            P("sp", "tp"),
            P("sp", "tp"),
            P("sp", "tp"),
            P(),
            P(None, "tp"),
            P(None, "tp"),
            P(None, "tp"),
            P("tp"),
            P("tp", None),
        ),
        out_specs=P(sp_tp, "grp", None),
        check_vma=False,
    )
```
